32 devices in a mesh: dp: 4 (over y, x), kv: 4 (over z), tp: 2 (over core).
Axes of the slice: x: 2, y: 2, z: 4, core: 2. Of those that a mesh axis runs over, the one named last changes fastest.
Arguments:
- tokens: bfloat16 [16, 2048], P('dp', 'kv'), may hold values from -700 to 700
- norm_gain: float32 [2048], P('kv'), may hold values from 0.1 to 1.9
- w_query: bfloat16 [2048, 2048], P('kv', 'tp'), may hold values from -0.25 to 0.25
- w_key: bfloat16 [2048, 2048], P('kv', 'tp'), may hold values from -0.125 to 0.125
- w_value: bfloat16 [2048, 2048], P('kv', 'tp'), may hold values from -0.125 to 0.125
- w_output: bfloat16 [2048, 2048], P('tp', 'kv'), may hold values from -0.125 to 0.125
- key_cache: bfloat16 [16, 2048, 16, 128], P('dp', 'kv', 'tp'), may hold values from -170 to 170
- value_cache: bfloat16 [16, 2048, 16, 128], P('dp', 'kv', 'tp'), may hold values from -6 to 6
- lengths: int32 [16], P('dp'), may hold values from 1024 to 2047, as said below
- lam: float32 [16], P('tp'), may hold values from 0.3 to 0.8
- head_gain: float32 [128], replicated, may hold values from 0.1 to 1.9
Outputs:
- attended: bfloat16 [16, 2048], P('dp', 'kv')
- new_key: bfloat16 [16, 2048], P('dp', 'tp')
- new_value: bfloat16 [16, 2048], P('dp', 'tp')
The draws below stay inside these ranges and needn't reach their ends.
Inputs may be any that keep to these rules, and one draw needn't show every extreme that they name: `lengths`: exactly one sequence, chosen by the draw, has 2047 past tokens.
All inputs are finite; a program needn't handle non-finite values.
Results may differ from the reference program's by a relative error of at most 0.012.
Values may be sent and summed in bfloat16 or wider, within the bound.
A program may use at most 64 MiB of HBM per device.

```python
import jax
import jax.numpy as jnp
from jax import lax

D = 2048
HEAD_COUNT = 16
HEAD_WIDTH = 64
POS_DEV = 512
VDIM = 128
BATCH = 16
CACHE_LENGTH = 2048
N_KV = 4
N_TP = 2


def draw_tokens(key, part):
    first = jax.random.fold_in(key, 11)
    second = jax.random.fold_in(key, 12)
    third = jax.random.fold_in(key, 13)
    column = jnp.arange(D, dtype=jnp.float32) / D
    base = jnp.clip(jax.random.normal(first, (BATCH, D), jnp.float32), -4.0, 4.0)
    scales = jnp.exp(2.3 * column + jax.random.uniform(second, (D,), jnp.float32, -0.5, 0.5))
    rows = jnp.exp(jax.random.uniform(third, (BATCH, 1), jnp.float32, 0.0, 2.3))
    return (base * scales[None, :] * rows).astype(jnp.bfloat16)


def draw_key_cache(key, part):
    first = jax.random.fold_in(key, 21)
    base = jnp.clip(jax.random.normal(first, (BATCH, CACHE_LENGTH, HEAD_COUNT, 2 * HEAD_WIDTH), jnp.float32), -4.0, 4.0)
    return base.astype(jnp.bfloat16)


def draw_lengths(key, part):
    first = jax.random.fold_in(key, 31)
    second = jax.random.fold_in(key, 32)
    short = jax.random.randint(first, (BATCH,), 1, CACHE_LENGTH // 2)
    values = CACHE_LENGTH - 1 - short
    chosen = jax.random.randint(second, (), 0, BATCH)
    leading = jnp.arange(BATCH, dtype=jnp.int32) == chosen
    return jnp.where(leading, CACHE_LENGTH - 1, values).astype(jnp.int32)


def steps_of(key, dims, cuts, smallest, top_value):
    gain, own = 1.0, jax.random.fold_in(key, 6)
    for dim, blocks in cuts:
        heights = jnp.exp(jax.random.uniform(jax.random.fold_in(own, dim), (blocks,), jnp.float32, smallest / len(cuts), top_value / len(cuts)))
        gain = gain * jnp.repeat(heights, dims[dim] // blocks).reshape([-1 if axis == dim else 1 for axis in range(len(dims))])
    return gain


def scatter_about(key, dims, scale, most, shards=(), held_as=jnp.bfloat16):
    entries = scale * jax.random.normal(key, dims, jnp.float32)
    if shards:
        entries = entries * steps_of(key, dims, shards, -0.22, 0.18)
    return jnp.clip(entries, -most, most).astype(held_as)


def setup_inputs(seed: int = 0) -> dict:
    key_of = jax.random.split(jax.random.key(seed), 12)
    return {
        "tokens": draw_tokens(jax.random.fold_in(key_of[11], 71), 0),
        "norm_gain": jnp.clip(1.0 + 0.18 * jax.random.normal(key_of[1], (D,), jnp.float32), 0.1, 1.9),
        "w_query": scatter_about(key_of[2], (D, HEAD_COUNT * 2 * HEAD_WIDTH), (1.75 / D ** 0.5), 0.25, ((0, 4), (1, 2))),
        "w_key": scatter_about(key_of[3], (D, HEAD_COUNT * 2 * HEAD_WIDTH), D ** -0.5, 0.125, ((0, 4), (1, 2))),
        "w_value": scatter_about(key_of[4], (D, HEAD_COUNT * VDIM), D ** -0.5, 0.125, ((0, 4), (1, 2))),
        "w_output": scatter_about(key_of[5], (HEAD_COUNT * VDIM, D), (HEAD_COUNT * VDIM) ** -0.5, 0.125, ((0, 2), (1, 4))),
        "key_cache": draw_key_cache(jax.random.fold_in(key_of[11], 71), 0),
        "value_cache": scatter_about(key_of[7], (BATCH, CACHE_LENGTH, HEAD_COUNT, VDIM), 1.0, 6.0, ((0, 4), (1, 4), (2, 2))),
        "lengths": draw_lengths(jax.random.fold_in(key_of[11], 71), 0),
        "lam": jnp.clip(0.3 + 0.5 * jax.random.uniform(key_of[9], (HEAD_COUNT,), jnp.float32) ** steps_of(key_of[9], (HEAD_COUNT,), ((0, 2),), -0.2, 0.2), 0.3, 0.8),
        "head_gain": jnp.clip(1.0 + 0.18 * jax.random.normal(key_of[10], (VDIM,), jnp.float32), 0.1, 1.9),
    }


epsilon = 1e-06

def reference(tokens, norm_gain, w_query, w_key, w_value, w_output, key_cache, value_cache, lengths, lam, head_gain):
    xfull = tokens.astype(jnp.float32)
    inv = lax.rsqrt(lax.optimization_barrier(jnp.mean(xfull * xfull, axis=-1, keepdims=True)) + epsilon)
    scaled = (xfull * norm_gain).astype(jnp.bfloat16)
    query = (jnp.dot(scaled, w_query, preferred_element_type=jnp.float32) * inv).astype(jnp.bfloat16)
    new_key = (jnp.dot(scaled, w_key, preferred_element_type=jnp.float32) * inv).astype(jnp.bfloat16)
    new_value = (jnp.dot(scaled, w_value, preferred_element_type=jnp.float32) * inv).astype(jnp.bfloat16)
    positions = jnp.arange(CACHE_LENGTH, dtype=jnp.int32)

    def one_sequence(items):
        key_cache_rows, vcache, query_row, krow, vrow, length = items
        hit = (positions == length)[:, None, None]
        key_rows = jnp.where(hit, krow.reshape(1, HEAD_COUNT, 2 * HEAD_WIDTH), key_cache_rows)
        values = jnp.where(hit, vrow.reshape(1, HEAD_COUNT, VDIM), vcache)
        logit_score = jnp.einsum('vcb,kvcb->vck', query_row.reshape(HEAD_COUNT, 2, HEAD_WIDTH).astype(jnp.float32), key_rows.reshape(CACHE_LENGTH, HEAD_COUNT, 2, HEAD_WIDTH).astype(jnp.float32)) * HEAD_WIDTH ** (-0.5)
        logit_score = logit_score.reshape(HEAD_COUNT, 2, N_KV, POS_DEV)
        live = (positions <= length).reshape(N_KV, POS_DEV)
        masked = jnp.where(live, logit_score, jnp.float32(-1e+30))
        block_peak = lax.optimization_barrier(jnp.max(masked, axis=-1))
        weights = jnp.where(live, jnp.exp(masked - block_peak[..., None]), jnp.float32(0.0))
        block_sum = lax.optimization_barrier(jnp.sum(weights, axis=-1))
        rounded = weights.astype(jnp.bfloat16).astype(jnp.float32)
        acc = jnp.einsum('hmnp,nphv->hmnv', rounded, values.reshape(N_KV, POS_DEV, HEAD_COUNT, VDIM).astype(jnp.float32))
        top = lax.optimization_barrier(jnp.max(block_peak, axis=-1))
        factor = jnp.exp(block_peak - top[..., None])
        total = lax.optimization_barrier(jnp.sum(block_sum * factor, axis=-1))
        summed = lax.optimization_barrier(jnp.sum(acc * factor[..., None], axis=2))
        return summed[:, 0] / total[:, 0, None] - lam[:, None] * summed[:, 1] / total[:, 1, None]
    mixed = lax.map(one_sequence, (key_cache, value_cache, query, new_key, new_value, lengths))
    heads = mixed * lax.rsqrt(lax.optimization_barrier(jnp.mean(mixed * mixed, axis=-1, keepdims=True)) + epsilon) * head_gain
    heads = heads.astype(jnp.bfloat16).reshape(BATCH, HEAD_COUNT * VDIM)
    half = HEAD_COUNT * VDIM // N_TP
    result = jnp.zeros((BATCH, D), jnp.float32)
    for member in range(N_TP):
        piece = jnp.dot(heads[:, member * half:(member + 1) * half], w_output[member * half:(member + 1) * half], preferred_element_type=jnp.float32).astype(jnp.bfloat16)
        result = result + piece.astype(jnp.float32)
    return (result.astype(jnp.bfloat16), new_key, new_value)
```

```python
import functools

import jax
import jax.numpy as jnp
from jax import lax
from jax.experimental import pallas as pl
from jax.experimental.pallas import tpu as pltpu
from jax.sharding import PartitionSpec as P

MESH = pl.DeviceIdType.MESH
epsilon = 1e-06
HBM = pl.ANY


def kernel(
    n, ntp, d_model, head_width,
    x_hbm, g_hbm, wq_hbm, wk_hbm, wv_hbm, wo_hbm, kc_hbm, vc_hbm, len_hbm, lam_hbm, hg_hbm,
    out_ref, nk_ref, nv_ref,
    x_s, g_s, wq_s, wk_s, wv_s, wo_s, kc_s, vc_s, len_s, lam_s, hg_s,
    q_all, kv_all, acc_all, stat_all, tp_all, bias_s, q_rows, k_rows, v_rows, head_rows,
    load_sem, k_sem, v_sem,
    q_send, q_recv, kv_send, kv_recv, acc_send, acc_recv, stat_send, stat_recv, tp_send, tp_recv,
):
    me = lax.axis_index("kv")
    side = lax.axis_index("tp")
    seqs = x_s.shape[0]
    width = wq_s.shape[1]
    vdim = hg_s.shape[1]
    heads = width // vdim
    cols = kc_s.shape[1]
    span = cols // heads
    f32 = jnp.float32

    def load(src, dst, i):
        copy = pltpu.make_async_copy(src, dst, load_sem.at[i])
        copy.start()
        return copy

    x_load = load(x_hbm, x_s, 0)
    g_load = load(g_hbm, g_s, 1)
    wq_load = load(wq_hbm, wq_s, 2)
    len_load = load(len_hbm, len_s, 3)
    wk_load = load(wk_hbm, wk_s, 4)
    wv_load = load(wv_hbm, wv_s, 5)
    lam_load = load(lam_hbm, lam_s, 6)
    hg_load = load(hg_hbm, hg_s, 7)

    barrier = pltpu.get_barrier_semaphore()
    for o in range(1, n):
        pl.semaphore_signal(
            barrier, inc=1, device_id={"kv": lax.rem(me + o, n)}, device_id_type=MESH
        )
    for o in range(1, ntp):
        pl.semaphore_signal(
            barrier, inc=1, device_id={"tp": lax.rem(side + o, ntp)}, device_id_type=MESH
        )

    def send_kv(buf, at, send, recv):
        for o in range(1, n):
            pltpu.make_async_remote_copy(
                src_ref=buf.at[at(me)], dst_ref=buf.at[at(me)],
                send_sem=send(o), recv_sem=recv(me),
                device_id={"kv": lax.rem(me + o, n)}, device_id_type=MESH,
            ).start()

    def wait_kv(buf, at, send, recv, sent):
        for o in range(1, n):
            src = lax.rem(me + o, n)
            copy = pltpu.make_async_remote_copy(
                src_ref=buf.at[at(src)], dst_ref=buf.at[at(src)],
                send_sem=send(o), recv_sem=recv(src),
                device_id={"kv": src}, device_id_type=MESH,
            )
            if sent:
                copy.wait_send()
            else:
                copy.wait_recv()

    x_load.wait()
    g_load.wait()
    xf = x_s[...].astype(f32)
    squares = jnp.sum(xf * xf, axis=-1, keepdims=True)
    scaled = (xf * g_s[...]).astype(jnp.bfloat16)
    wq_load.wait()
    k_loads, v_loads = [], []
    for b in range(seqs):
        copy = pltpu.make_async_copy(kc_hbm.at[b], kc_s.at[b], k_sem.at[b])
        copy.start()
        k_loads.append(copy)
    for b in range(seqs):
        copy = pltpu.make_async_copy(vc_hbm.at[b], vc_s.at[b], v_sem.at[b])
        copy.start()
        v_loads.append(copy)
    wo_load = load(wo_hbm, wo_s, 8)

    q_all[me, :, :width] = jnp.dot(scaled, wq_s[...], preferred_element_type=f32)
    q_all[me, :, width:] = jnp.broadcast_to(squares, (seqs, q_all.shape[2] - width))
    pl.semaphore_wait(barrier, n - 1 + ntp - 1)
    whole = lambda s: s
    q_args = (q_all, whole, lambda o: q_send.at[o], lambda s: q_recv.at[s])
    kv_args = (kv_all, whole, lambda o: kv_send.at[o], lambda s: kv_recv.at[s])
    stat_args = (stat_all, whole, lambda o: stat_send.at[o], lambda s: stat_recv.at[s])
    acc_args = [
        (
            acc_all,
            lambda s, b=b: (s, b),
            lambda o, b=b: acc_send.at[o, b],
            lambda s, b=b: acc_recv.at[s, b],
        )
        for b in range(seqs)
    ]
    send_kv(*q_args)
    wk_load.wait()
    kv_all[me, :, :width] = jnp.dot(scaled, wk_s[...], preferred_element_type=f32)
    wv_load.wait()
    kv_all[me, :, width:] = jnp.dot(scaled, wv_s[...], preferred_element_type=f32)
    send_kv(*kv_args)

    len_load.wait()
    lam_load.wait()
    hg_load.wait()
    col = lax.broadcasted_iota(jnp.int32, (2 * heads, cols), 1)
    row = lax.broadcasted_iota(jnp.int32, (2 * heads, cols), 0)
    diagonal = lax.rem(col, heads) == lax.rem(row, heads)
    local = [len_s[b] - me * span for b in range(seqs)]
    for b in range(seqs):
        bias_s[b] = jnp.where(diagonal & (col < local[b] * heads), f32(0.0), f32(-jnp.inf))
    lane = lax.broadcasted_iota(jnp.int32, (2 * heads, vdim), 1)
    half = lax.broadcasted_iota(jnp.int32, (2 * heads, vdim), 0) // heads
    own_map = (lane // head_width) == half

    wait_kv(*q_args, False)
    total = q_all[0]
    for s in range(1, n):
        total = total + q_all[s]
    inv = lax.rsqrt(total[:, width : width + 1] / d_model + epsilon)
    query = (total[:, :width] * inv).astype(jnp.bfloat16).astype(f32)
    for h in range(heads):
        q_rows[:, h, :] = query[:, h * vdim : (h + 1) * vdim]

    def doubled(rows):
        return jnp.concatenate([rows, rows], axis=0)

    queries, scores = [], []
    for b in range(seqs):
        q_b = jnp.where(own_map, doubled(q_rows[b]), f32(0.0))
        queries.append(q_b)
    for b in range(seqs):
        k_loads[b].wait()
        scores.append(
            lax.dot_general(
                (queries[b] * head_width**-0.5).astype(jnp.bfloat16), kc_s[b],
                (((1,), (1,)), ((), ())), preferred_element_type=f32,
            )
            + bias_s[b]
        )
        bias_s[b] = scores[b]

    wait_kv(*kv_args, False)
    total = kv_all[0]
    for s in range(1, n):
        total = total + kv_all[s]
    fresh = (total * inv).astype(jnp.bfloat16)
    nk_ref[...] = fresh[:, :width]
    nv_ref[...] = fresh[:, width:]
    fresh = fresh.astype(f32)
    for h in range(heads):
        k_rows[:, h, :] = fresh[:, h * vdim : (h + 1) * vdim]
        v_rows[:, h, :] = fresh[:, width + h * vdim : width + (h + 1) * vdim]

    stats = jnp.zeros((2 * heads, stat_all.shape[2]), f32)
    stat_lane = lax.broadcasted_iota(jnp.int32, stats.shape, 1)
    for b in range(seqs):
        new_score = jnp.sum(queries[b] * doubled(k_rows[b]), axis=-1, keepdims=True)
        here = (local[b] >= 0) & (local[b] < span)
        new_score = jnp.where(here, new_score * head_width**-0.5, f32(-jnp.inf))
        score = bias_s[b]
        peak = jnp.maximum(jnp.max(score, axis=-1, keepdims=True), new_score)
        peak = jnp.maximum(peak, f32(-1e30))
        weights = jnp.exp(score - peak)
        new_weight = jnp.exp(new_score - peak)
        block_sum = jnp.sum(weights, axis=-1, keepdims=True) + new_weight
        v_loads[b].wait()
        acc = jnp.dot(weights.astype(jnp.bfloat16), vc_s[b], preferred_element_type=f32)
        acc_all[me, b] = acc + new_weight.astype(jnp.bfloat16).astype(f32) * doubled(v_rows[b])
        send_kv(*acc_args[b])
        stats = jnp.where(stat_lane == b, peak, stats)
        stats = jnp.where(stat_lane == seqs + b, block_sum, stats)
    stat_all[me] = stats
    send_kv(*stat_args)

    h_row = lax.broadcasted_iota(jnp.int32, (heads, 1), 0)
    lam = jnp.zeros((heads, 1), f32)
    for h in range(heads):
        lam = jnp.where(h_row == h, lam_s[h], lam)

    wait_kv(*stat_args, False)
    for b in range(seqs):
        peaks = [stat_all[s][:, b : b + 1] for s in range(n)]
        sums = [stat_all[s][:, seqs + b : seqs + b + 1] for s in range(n)]
        top = functools.reduce(jnp.maximum, peaks)
        factors = [jnp.exp(p - top) for p in peaks]
        whole_sum = sum(l * f for l, f in zip(sums, factors))
        wait_kv(*acc_args[b], False)
        summed = acc_all[0, b] * factors[0]
        for s in range(1, n):
            summed = summed + acc_all[s, b] * factors[s]
        maps = summed / whole_sum
        mixed = maps[:heads] - lam * maps[heads:]
        normed = (
            mixed
            * lax.rsqrt(jnp.mean(mixed * mixed, axis=-1, keepdims=True) + epsilon)
            * hg_s[...]
        )
        head_rows[b] = normed
    flat = jnp.concatenate(
        [head_rows[:, h, :].astype(jnp.bfloat16) for h in range(heads)], axis=-1
    )
    wo_load.wait()
    tp_all[side] = jnp.dot(flat, wo_s[...], preferred_element_type=f32).astype(jnp.bfloat16)
    for o in range(1, ntp):
        pltpu.make_async_remote_copy(
            src_ref=tp_all.at[side], dst_ref=tp_all.at[side],
            send_sem=tp_send.at[o], recv_sem=tp_recv.at[side],
            device_id={"tp": lax.rem(side + o, ntp)}, device_id_type=MESH,
        ).start()
    wait_kv(*q_args, True)
    wait_kv(*kv_args, True)
    wait_kv(*stat_args, True)
    for b in range(seqs):
        wait_kv(*acc_args[b], True)
    for o in range(1, ntp):
        src = lax.rem(side + o, ntp)
        copy = pltpu.make_async_remote_copy(
            src_ref=tp_all.at[src], dst_ref=tp_all.at[src],
            send_sem=tp_send.at[o], recv_sem=tp_recv.at[src],
            device_id={"tp": src}, device_id_type=MESH,
        )
        copy.wait_recv()
        copy.wait_send()
    result = tp_all[0].astype(f32)
    for s in range(1, ntp):
        result = result + tp_all[s].astype(f32)
    out_ref[...] = result.astype(jnp.bfloat16)


def per_device(
    n, ntp,
    tokens, norm_gain, w_query, w_key, w_value, w_output,
    key_cache, value_cache, lengths, lam, head_gain,
):
    seqs, features = tokens.shape
    width = w_query.shape[1]
    heads = lam.shape[0]
    vdim = head_gain.shape[0]
    span = key_cache.shape[1]
    columns = w_output.shape[1]
    bf16, f32 = jnp.bfloat16, jnp.float32
    vmem, dma = pltpu.VMEM, pltpu.SemaphoreType.DMA
    keys = key_cache.reshape(seqs, span * heads, vdim)
    values = value_cache.reshape(seqs, span * heads, vdim)
    body = functools.partial(kernel, n, ntp, features * n, vdim // 2)
    return pl.pallas_call(
        body,
        out_shape=(
            jax.ShapeDtypeStruct((seqs, columns), bf16),
            jax.ShapeDtypeStruct((seqs, width), bf16),
            jax.ShapeDtypeStruct((seqs, width), bf16),
        ),
        in_specs=[pl.BlockSpec(memory_space=HBM)] * 11,
        out_specs=(pl.BlockSpec(memory_space=pltpu.VMEM),) * 3,
        scratch_shapes=[
            vmem((seqs, features), bf16),
            vmem((1, features), f32),
            vmem(w_query.shape, bf16),
            vmem(w_key.shape, bf16),
            vmem(w_value.shape, bf16),
            vmem(w_output.shape, bf16),
            vmem(keys.shape, bf16),
            vmem(values.shape, bf16),
            pltpu.SMEM((seqs,), jnp.int32),
            pltpu.SMEM((heads,), f32),
            vmem((1, vdim), f32),
            vmem((n, seqs, width + 128), f32),
            vmem((n, seqs, 2 * width), f32),
            vmem((n, seqs, 2 * heads, vdim), f32),
            vmem((n, 2 * heads, 128), f32),
            vmem((ntp, seqs, columns), bf16),
            vmem((seqs, 2 * heads, span * heads), f32),
            vmem((seqs, heads, vdim), f32),
            vmem((seqs, heads, vdim), f32),
            vmem((seqs, heads, vdim), f32),
            vmem((seqs, heads, vdim), f32),
            dma((9,)), dma((seqs,)), dma((seqs,)),
            dma((n,)), dma((n,)), dma((n,)), dma((n,)),
            dma((n, seqs)), dma((n, seqs)), dma((n,)), dma((n,)),
            dma((ntp,)), dma((ntp,)),
        ],
        compiler_params=pltpu.CompilerParams(
            collective_id=0, has_side_effects=True, vmem_limit_bytes=56 * 1024 * 1024
        ),
    )(
        tokens, norm_gain.reshape(1, -1), w_query, w_key, w_value, w_output,
        keys, values, lengths, lam, head_gain.reshape(1, -1),
    )


def solution(mesh):
    in_specs = (
        P("dp", "kv"),
        P("kv"),
        P("kv", "tp"),
        P("kv", "tp"),
        P("kv", "tp"),
        P("tp", "kv"),
        P("dp", "kv", "tp", None),
        P("dp", "kv", "tp", None),
        P("dp"),
        P("tp"),
        P(),
    )
    out_specs = (P("dp", "kv"), P("dp", "tp"), P("dp", "tp"))
    return jax.shard_map(
        functools.partial(per_device, mesh.shape["kv"], mesh.shape["tp"]),
        mesh=mesh, in_specs=in_specs, out_specs=out_specs, check_vma=False,
    )
```

```python
import functools

import jax
import jax.numpy as jnp
from jax import lax
from jax.experimental import pallas as pl
from jax.experimental.pallas import tpu as pltpu
from jax.sharding import PartitionSpec as P

MESH = pl.DeviceIdType.MESH
epsilon = 1e-06
HBM = pltpu.HBM


def kernel(
    n, ntp, d_model, head_width,
    x_hbm, g_hbm, wq_hbm, wk_hbm, wv_hbm, wo_hbm, kc_hbm, vc_hbm, len_hbm, lam_hbm, hg_hbm,
    out_ref, nk_ref, nv_ref,
    x_s, g_s, wq_s, wk_s, wv_s, wo_s, kc_s, vc_s, len_s, lam_s, hg_s,
    q_all, kv_part, kv_in, kv_out, acc_all, stat_all, tp_all, bias_s, q_rows, fresh_s, head_rows,
    load_sem, k_sem, v_sem,
    q_send, q_recv, part_send, part_recv, kv_send, kv_recv, acc_send, acc_recv, stat_send, stat_recv, tp_send, tp_recv,
):
    me = lax.axis_index("kv")
    side = lax.axis_index("tp")
    seqs = x_s.shape[0]
    width = wq_s.shape[1]
    vdim = hg_s.shape[1]
    heads = width // vdim
    cols = kc_s.shape[1]
    span = cols // heads
    f32 = jnp.float32

    def load(src, dst, i):
        copy = pltpu.make_async_copy(src, dst, load_sem.at[i])
        copy.start()
        return copy

    x_load = load(x_hbm, x_s, 0)
    g_load = load(g_hbm, g_s, 1)
    wq_load = load(wq_hbm, wq_s, 2)
    len_load = load(len_hbm, len_s, 3)
    wk_load = load(wk_hbm, wk_s, 4)
    wv_load = load(wv_hbm, wv_s, 5)
    lam_load = load(lam_hbm, lam_s, 6)
    hg_load = load(hg_hbm, hg_s, 7)

    barrier = pltpu.get_barrier_semaphore()
    for o in range(1, n):
        pl.semaphore_signal(
            barrier, inc=1, device_id={"kv": lax.rem(me + o, n)}, device_id_type=MESH
        )
    for o in range(1, ntp):
        pl.semaphore_signal(
            barrier, inc=1, device_id={"tp": lax.rem(side + o, ntp)}, device_id_type=MESH
        )

    def send_kv(buf, at, send, recv):
        for o in range(1, n):
            pltpu.make_async_remote_copy(
                src_ref=buf.at[at(me)], dst_ref=buf.at[at(me)],
                send_sem=send(o), recv_sem=recv(me),
                device_id={"kv": lax.rem(me + o, n)}, device_id_type=MESH,
            ).start()

    def wait_kv(buf, at, send, recv, sent, offsets=range(1, n)):
        for o in offsets:
            src = lax.rem(me + o, n)
            copy = pltpu.make_async_remote_copy(
                src_ref=buf.at[at(src)], dst_ref=buf.at[at(src)],
                send_sem=send(o), recv_sem=recv(src),
                device_id={"kv": src}, device_id_type=MESH,
            )
            if sent:
                copy.wait_send()
            else:
                copy.wait_recv()

    x_load.wait()
    g_load.wait()
    xf = x_s[...].astype(f32)
    squares = jnp.sum(xf * xf, axis=-1, keepdims=True)
    scaled = (xf * g_s[...]).astype(jnp.bfloat16)
    wq_load.wait()
    k_loads, v_loads = [], []
    for b in range(seqs):
        copy = pltpu.make_async_copy(kc_hbm.at[b], kc_s.at[b], k_sem.at[b])
        copy.start()
        k_loads.append(copy)
    for b in range(seqs):
        copy = pltpu.make_async_copy(vc_hbm.at[b], vc_s.at[b], v_sem.at[b])
        copy.start()
        v_loads.append(copy)
    wo_load = load(wo_hbm, wo_s, 8)

    q_all[me, :, :width] = jnp.dot(scaled, wq_s[...], preferred_element_type=f32)
    q_all[me, :, width:] = jnp.broadcast_to(squares, (seqs, q_all.shape[2] - width))
    pl.semaphore_wait(barrier, n - 1 + ntp - 1)
    whole = lambda s: s
    q_args = (q_all, whole, lambda o: q_send.at[o], lambda s: q_recv.at[s])
    kv_args = (kv_out, whole, lambda o: kv_send.at[o], lambda s: kv_recv.at[s])
    stat_args = (stat_all, whole, lambda o: stat_send.at[o], lambda s: stat_recv.at[s])
    acc_args = [
        (
            acc_all,
            lambda s, b=b: (s, b),
            lambda o, b=b: acc_send.at[o, b],
            lambda s, b=b: acc_recv.at[s, b],
        )
        for b in range(seqs)
    ]
    send_kv(*q_args)
    units = kv_part.shape[1]

    def keep_part(part, first):
        for h in range(heads):
            slab = part[:, h * vdim : (h + 1) * vdim]
            at = (first + h) * seqs
            step = min(seqs, units)
            for r in range(0, seqs, step):
                kv_part[(at + r) // units, pl.ds((at + r) % units, step), :] = slab[r : r + step]

    wk_load.wait()
    keep_part(jnp.dot(scaled, wk_s[...], preferred_element_type=f32), 0)
    wv_load.wait()
    keep_part(jnp.dot(scaled, wv_s[...], preferred_element_type=f32), heads)

    len_load.wait()
    lam_load.wait()
    hg_load.wait()
    col = lax.broadcasted_iota(jnp.int32, (2 * heads, cols), 1)
    row = lax.broadcasted_iota(jnp.int32, (2 * heads, cols), 0)
    diagonal = lax.rem(col, heads) == lax.rem(row, heads)
    for b in range(seqs):
        before = (len_s[b] - me * span) * heads
        bias_s[b] = jnp.where(diagonal & (col < before), f32(0.0), f32(-jnp.inf))
    lane = lax.broadcasted_iota(jnp.int32, (2 * heads, vdim), 1)
    half = lax.broadcasted_iota(jnp.int32, (2 * heads, vdim), 0) // heads
    own_map = (lane // head_width) == half

    wait_kv(*q_args, False, range(1, 2))

    def part_copy(o, sent):
        peer = lax.rem(me + o, n)
        slot = me if sent else peer
        return pltpu.make_async_remote_copy(
            src_ref=kv_part.at[peer], dst_ref=kv_in.at[slot],
            send_sem=part_send.at[o], recv_sem=part_recv.at[slot],
            device_id={"kv": peer}, device_id_type=MESH,
        )

    for o in range(1, n):
        part_copy(o, True).start()
    wait_kv(*q_args, False, range(2, n))
    for b in range(seqs):
        k_loads[b].wait()
        v_loads[b].wait()
    total = q_all[0]
    for s in range(1, n):
        total = total + q_all[s]
    inv = lax.rsqrt(total[:, width : width + 1] / d_model + epsilon)
    query = (total[:, :width] * inv).astype(jnp.bfloat16).astype(f32)
    for h in range(heads):
        q_rows[:, h, :] = query[:, h * vdim : (h + 1) * vdim]

    def doubled(rows):
        return jnp.concatenate([rows, rows], axis=0)

    queries = [
        jnp.where(own_map, doubled(q_rows[b]), f32(0.0)) * head_width**-0.5 for b in range(seqs)
    ]
    stats = jnp.zeros(stat_all.shape[1:], f32)
    stat_lane = lax.broadcasted_iota(jnp.int32, stats.shape, 1)
    for b in range(seqs):
        score = (
            lax.dot_general(
                queries[b].astype(jnp.bfloat16), kc_s[b],
                (((1,), (1,)), ((), ())), preferred_element_type=f32,
            )
            + bias_s[b]
        )
        peak = jnp.maximum(jnp.max(score, axis=-1, keepdims=True), f32(-1e30))
        weights = jnp.exp(score - peak)
        block_sum = jnp.sum(weights, axis=-1, keepdims=True)
        acc = jnp.dot(weights.astype(jnp.bfloat16), vc_s[b], preferred_element_type=f32)
        acc_all[me, b] = acc.astype(acc_all.dtype)
        send_kv(*acc_args[b])
        for j in range(2):
            rows = slice(j * heads, (j + 1) * heads)
            stats = jnp.where(stat_lane == 2 * b + j, peak[rows], stats)
            stats = jnp.where(stat_lane == 2 * (seqs + b) + j, block_sum[rows], stats)
        if b == seqs - 1:
            stat_all[me] = stats
            send_kv(*stat_args)
        if b == (seqs - 1) // 2:
            share = kv_part[me]
            for o in range(1, n):
                part_copy(o, False).wait_recv()
                share = share + kv_in[lax.rem(me + o, n)]
            unit = me * units + lax.broadcasted_iota(jnp.int32, (units, 1), 0)
            seq = lax.rem(unit, seqs)
            scale = jnp.zeros((units, 1), f32)
            for c in range(seqs):
                scale = jnp.where(seq == c, inv[c : c + 1], scale)
            kv_out[me] = (share * scale).astype(jnp.bfloat16)
            send_kv(*kv_args)

    h_row = lax.broadcasted_iota(jnp.int32, (heads, 1), 0)
    lam = jnp.zeros((heads, 1), f32)
    for h in range(heads):
        lam = jnp.where(h_row == h, lam_s[h], lam)

    wait_kv(*kv_args, False)
    for s in range(n):
        fresh_s[pl.ds(s * units, units), :] = kv_out[s].astype(f32)
    for h in range(heads):
        place = slice(h * vdim, (h + 1) * vdim)
        nk_ref[:, place] = fresh_s[pl.ds(h * seqs, seqs), :].astype(jnp.bfloat16)
        nv_ref[:, place] = fresh_s[pl.ds((heads + h) * seqs, seqs), :].astype(jnp.bfloat16)

    new_scores, new_values = [], []
    for b in range(seqs):
        new_key = doubled(fresh_s[pl.ds(b, heads, stride=seqs), :])
        new_values.append(doubled(fresh_s[pl.ds(heads * seqs + b, heads, stride=seqs), :]))
        new_scores.append(jnp.sum(queries[b] * new_key, axis=-1, keepdims=True))

    wait_kv(*stat_args, False)

    def stat(s, i):
        return jnp.concatenate([stat_all[s][:, 2 * i + j : 2 * i + j + 1] for j in range(2)], axis=0)

    weighted = []
    for b in range(seqs):
        peaks = [stat(s, b) for s in range(n)]
        top = functools.reduce(jnp.maximum, peaks, new_scores[b])
        factors = [jnp.exp(p - top) for p in peaks]
        new_factor = jnp.exp(new_scores[b] - top)
        whole_sum = new_factor
        for s in range(n):
            whole_sum = whole_sum + stat(s, seqs + b) * factors[s]
        weighted.append((factors, new_factor, whole_sum))
    for b in range(seqs):
        wait_kv(*acc_args[b], False)
    for b in range(seqs):
        factors, new_factor, whole_sum = weighted[b]
        summed = new_values[b] * new_factor
        for s in range(n):
            summed = summed + acc_all[s, b].astype(f32) * factors[s]
        maps = summed / whole_sum
        mixed = maps[:heads] - lam * maps[heads:]
        normed = (
            mixed
            * lax.rsqrt(jnp.mean(mixed * mixed, axis=-1, keepdims=True) + epsilon)
            * hg_s[...]
        )
        head_rows[b] = normed
    flat = jnp.concatenate(
        [head_rows[:, h, :].astype(jnp.bfloat16) for h in range(heads)], axis=-1
    )
    wo_load.wait()
    tp_all[side] = jnp.dot(flat, wo_s[...], preferred_element_type=f32).astype(jnp.bfloat16)
    for o in range(1, ntp):
        pltpu.make_async_remote_copy(
            src_ref=tp_all.at[side], dst_ref=tp_all.at[side],
            send_sem=tp_send.at[o], recv_sem=tp_recv.at[side],
            device_id={"tp": lax.rem(side + o, ntp)}, device_id_type=MESH,
        ).start()
    wait_kv(*q_args, True)
    for o in range(1, n):
        part_copy(o, True).wait_send()
    wait_kv(*kv_args, True)
    wait_kv(*stat_args, True)
    for b in range(seqs):
        wait_kv(*acc_args[b], True)
    for o in range(1, ntp):
        src = lax.rem(side + o, ntp)
        copy = pltpu.make_async_remote_copy(
            src_ref=tp_all.at[src], dst_ref=tp_all.at[src],
            send_sem=tp_send.at[o], recv_sem=tp_recv.at[src],
            device_id={"tp": src}, device_id_type=MESH,
        )
        copy.wait_recv()
        copy.wait_send()
    result = tp_all[0].astype(f32)
    for s in range(1, ntp):
        result = result + tp_all[s].astype(f32)
    out_ref[...] = result.astype(jnp.bfloat16)


def store(a_ref, b_ref, c_ref, a_out, b_out, c_out, sem):
    pairs = ((a_ref, a_out), (b_ref, b_out), (c_ref, c_out))
    copies = [pltpu.make_async_copy(src, dst, sem.at[i]) for i, (src, dst) in enumerate(pairs)]
    for copy in copies:
        copy.start()
    for copy in copies:
        copy.wait()


def per_device(
    n, ntp,
    tokens, norm_gain, w_query, w_key, w_value, w_output,
    key_cache, value_cache, lengths, lam, head_gain,
):
    seqs, features = tokens.shape
    width = w_query.shape[1]
    heads = lam.shape[0]
    vdim = head_gain.shape[0]
    span = key_cache.shape[1]
    columns = w_output.shape[1]
    bf16, f32 = jnp.bfloat16, jnp.float32
    vmem, dma = pltpu.VMEM, pltpu.SemaphoreType.DMA
    keys = key_cache.reshape(seqs, span * heads, vdim)
    values = value_cache.reshape(seqs, span * heads, vdim)
    units = 2 * heads * seqs // n
    body = functools.partial(kernel, n, ntp, features * n, vdim // 2)
    shapes = ((seqs, columns), (seqs, width), (seqs, width))
    parts = pl.pallas_call(
        body,
        out_shape=tuple(vmem(shape, bf16) for shape in shapes),
        in_specs=[pl.BlockSpec(memory_space=HBM)] * 11,
        out_specs=(pl.BlockSpec(memory_space=pltpu.VMEM),) * 3,
        scratch_shapes=[
            vmem((seqs, features), bf16),
            vmem((1, features), f32),
            vmem(w_query.shape, bf16),
            vmem(w_key.shape, bf16),
            vmem(w_value.shape, bf16),
            vmem(w_output.shape, bf16),
            vmem(keys.shape, bf16),
            vmem(values.shape, bf16),
            pltpu.SMEM((seqs,), jnp.int32),
            pltpu.SMEM((heads,), f32),
            vmem((1, vdim), f32),
            vmem((n, seqs, width + 128), f32),
            vmem((n, units, vdim), f32),
            vmem((n, units, vdim), f32),
            vmem((n, units, vdim), bf16),
            vmem((n, seqs, 2 * heads, vdim), bf16),
            vmem((n, heads, 128), f32),
            vmem((ntp, seqs, columns), bf16),
            vmem((seqs, 2 * heads, span * heads), f32),
            vmem((seqs, heads, vdim), f32),
            vmem((2 * heads * seqs, vdim), f32),
            vmem((seqs, heads, vdim), f32),
            dma((9,)), dma((seqs,)), dma((seqs,)),
            dma((n,)), dma((n,)), dma((n,)), dma((n,)), dma((n,)), dma((n,)),
            dma((n, seqs)), dma((n, seqs)), dma((n,)), dma((n,)),
            dma((ntp,)), dma((ntp,)),
        ],
        compiler_params=pltpu.CompilerParams(
            collective_id=0, has_side_effects=True, vmem_limit_bytes=56 * 1024 * 1024
        ),
    )(
        tokens, norm_gain.reshape(1, -1), w_query, w_key, w_value, w_output,
        keys, values, lengths, lam, head_gain.reshape(1, -1),
    )
    return pl.pallas_call(
        store,
        out_shape=tuple(jax.ShapeDtypeStruct(shape, bf16) for shape in shapes),
        in_specs=[pl.BlockSpec(memory_space=pltpu.VMEM)] * 3,
        out_specs=(pl.BlockSpec(memory_space=HBM),) * 3,
        scratch_shapes=[dma((3,))],
        compiler_params=pltpu.CompilerParams(vmem_limit_bytes=1024 * 1024),
    )(*parts)


def solution(mesh):
    in_specs = (
        P("dp", "kv"),
        P("kv"),
        P("kv", "tp"),
        P("kv", "tp"),
        P("kv", "tp"),
        P("tp", "kv"),
        P("dp", "kv", "tp", None),
        P("dp", "kv", "tp", None),
        P("dp"),
        P("tp"),
        P(),
    )
    out_specs = (P("dp", "kv"), P("dp", "tp"), P("dp", "tp"))
    return jax.shard_map(
        functools.partial(per_device, mesh.shape["kv"], mesh.shape["tp"]),
        mesh=mesh, in_specs=in_specs, out_specs=out_specs, check_vma=False,
    )
```

```python
import functools

import jax
import jax.numpy as jnp
from jax import lax
from jax.experimental import pallas as pl
from jax.experimental.pallas import tpu as pltpu
from jax.sharding import PartitionSpec as P

MESH = pl.DeviceIdType.MESH
epsilon = 1e-06
HBM = pltpu.HBM


def kernel(
    n, ntp, d_model, head_width,
    x_hbm, g_hbm, wq_hbm, wk_hbm, wv_hbm, wo_hbm, kc_hbm, vc_hbm, len_hbm, lam_hbm, hg_hbm,
    out_ref, nk_ref, nv_ref,
    x_s, g_s, wq_s, wk_s, wv_s, wo_s, kc_s, vc_s, len_s, lam_s, hg_s,
    q_all, kv_all, acc_all, stat_all, tp_all, bias_s, q_rows, fresh_s, head_rows,
    load_sem, k_sem, v_sem,
    q_send, q_recv, kv_send, kv_recv, acc_send, acc_recv, stat_send, stat_recv, tp_send, tp_recv,
):
    me = lax.axis_index("kv")
    side = lax.axis_index("tp")
    seqs = x_s.shape[0]
    width = wq_s.shape[1]
    vdim = hg_s.shape[1]
    heads = width // vdim
    cols = kc_s.shape[1]
    span = cols // heads
    f32 = jnp.float32

    def load(src, dst, i):
        copy = pltpu.make_async_copy(src, dst, load_sem.at[i])
        copy.start()
        return copy

    x_load = load(x_hbm, x_s, 0)
    g_load = load(g_hbm, g_s, 1)
    wq_load = load(wq_hbm, wq_s, 2)

    barrier = pltpu.get_barrier_semaphore()
    for o in range(1, n):
        pl.semaphore_signal(
            barrier, inc=1, device_id={"kv": lax.rem(me + o, n)}, device_id_type=MESH
        )
    for o in range(1, ntp):
        pl.semaphore_signal(
            barrier, inc=1, device_id={"tp": lax.rem(side + o, ntp)}, device_id_type=MESH
        )

    def far_peer(o):
        k = o - 1
        down = n - 1 - k - lax.div(me + k, n - 1)
        up = k + lax.div(k - me + n, n)
        return down + lax.div(2 * me, n) * (up - down)

    def send_kv(buf, at, send, recv):
        for o in range(1, n):
            pltpu.make_async_remote_copy(
                src_ref=buf.at[at(me)], dst_ref=buf.at[at(me)],
                send_sem=send(o), recv_sem=recv(me),
                device_id={"kv": far_peer(o)}, device_id_type=MESH,
            ).start()

    def wait_kv(buf, at, send, recv, sent, offsets=range(1, n)):
        for o in offsets:
            src = lax.rem(me + o, n)
            copy = pltpu.make_async_remote_copy(
                src_ref=buf.at[at(src)], dst_ref=buf.at[at(src)],
                send_sem=send(o), recv_sem=recv(src),
                device_id={"kv": src}, device_id_type=MESH,
            )
            if sent:
                copy.wait_send()
            else:
                copy.wait_recv()

    x_load.wait()
    g_load.wait()
    xf = x_s[...].astype(f32)
    squares = jnp.sum(xf * xf, axis=-1, keepdims=True)
    scaled = (xf * g_s[...]).astype(jnp.bfloat16)
    wq_load.wait()
    wk_load = load(wk_hbm, wk_s, 4)
    wv_load = load(wv_hbm, wv_s, 5)
    len_load = load(len_hbm, len_s, 3)
    lam_load = load(lam_hbm, lam_s, 6)
    hg_load = load(hg_hbm, hg_s, 7)
    k_loads, v_loads = [], []
    for b in range(seqs):
        copy = pltpu.make_async_copy(kc_hbm.at[b], kc_s.at[b], k_sem.at[b])
        copy.start()
        k_loads.append(copy)
    for b in range(seqs):
        copy = pltpu.make_async_copy(vc_hbm.at[b], vc_s.at[b], v_sem.at[b])
        copy.start()
        v_loads.append(copy)
    wo_load = load(wo_hbm, wo_s, 8)

    q_all[me, :, :width] = jnp.dot(scaled, wq_s[...], preferred_element_type=f32)
    q_all[me, :, width:] = jnp.broadcast_to(squares, (seqs, q_all.shape[2] - width))
    pl.semaphore_wait(barrier, n - 1 + ntp - 1)
    whole = lambda s: s
    q_args = (q_all, whole, lambda o: q_send.at[o], lambda s: q_recv.at[s])
    kv_args = (kv_all, whole, lambda o: kv_send.at[o], lambda s: kv_recv.at[s])
    stat_args = (stat_all, whole, lambda o: stat_send.at[o], lambda s: stat_recv.at[s])
    acc_args = [
        (
            acc_all,
            lambda s, b=b: (s, b),
            lambda o, b=b: acc_send.at[o, b],
            lambda s, b=b: acc_recv.at[s, b],
        )
        for b in range(seqs)
    ]
    send_kv(*q_args)
    wk_load.wait()
    kv_all[me, :, :width] = jnp.dot(scaled, wk_s[...], preferred_element_type=f32)
    wv_load.wait()
    kv_all[me, :, width:] = jnp.dot(scaled, wv_s[...], preferred_element_type=f32)

    len_load.wait()
    lam_load.wait()
    hg_load.wait()
    col = lax.broadcasted_iota(jnp.int32, (2 * heads, cols), 1)
    row = lax.broadcasted_iota(jnp.int32, (2 * heads, cols), 0)
    diagonal = lax.rem(col, heads) == lax.rem(row, heads)
    for b in range(seqs):
        before = (len_s[b] - me * span) * heads
        bias_s[b] = jnp.where(diagonal & (col < before), f32(0.0), f32(-jnp.inf))
    lane = lax.broadcasted_iota(jnp.int32, (2 * heads, vdim), 1)
    half = lax.broadcasted_iota(jnp.int32, (2 * heads, vdim), 0) // heads
    own_map = (lane // head_width) == half

    wait_kv(*q_args, False, range(1, 2))

    send_kv(*kv_args)
    wait_kv(*q_args, False, range(2, n))
    for b in range(seqs):
        k_loads[b].wait()
        v_loads[b].wait()
    total = q_all[0]
    for s in range(1, n):
        total = total + q_all[s]
    inv = lax.rsqrt(total[:, width : width + 1] / d_model + epsilon)
    query = (total[:, :width] * inv).astype(jnp.bfloat16).astype(f32)
    for h in range(heads):
        q_rows[:, h, :] = query[:, h * vdim : (h + 1) * vdim]

    def doubled(rows):
        return jnp.concatenate([rows, rows], axis=0)

    queries = [
        jnp.where(own_map, doubled(q_rows[b]), f32(0.0)) * head_width**-0.5 for b in range(seqs)
    ]
    stats = jnp.zeros(stat_all.shape[1:], f32)
    stat_lane = lax.broadcasted_iota(jnp.int32, stats.shape, 1)
    rounded = []
    for b in range(seqs):
        score = (
            lax.dot_general(
                queries[b].astype(jnp.bfloat16), kc_s[b],
                (((1,), (1,)), ((), ())), preferred_element_type=f32,
            )
            + bias_s[b]
        )
        peak = jnp.maximum(jnp.max(score, axis=-1, keepdims=True), f32(-1e30))
        weights = jnp.exp(score - peak)
        block_sum = jnp.sum(weights, axis=-1, keepdims=True)
        rounded.append(weights.astype(jnp.bfloat16))
        for j in range(2):
            rows = slice(j * heads, (j + 1) * heads)
            stats = jnp.where(stat_lane == 2 * b + j, peak[rows], stats)
            stats = jnp.where(stat_lane == 2 * (seqs + b) + j, block_sum[rows], stats)
    stat_all[me] = stats
    send_kv(*stat_args)
    for b in range(seqs):
        acc = jnp.dot(rounded[b], vc_s[b], preferred_element_type=f32)
        acc_all[me, b] = acc.astype(acc_all.dtype)
        send_kv(*acc_args[b])

    h_row = lax.broadcasted_iota(jnp.int32, (heads, 1), 0)
    lam = jnp.zeros((heads, 1), f32)
    for h in range(heads):
        lam = jnp.where(h_row == h, lam_s[h], lam)

    wait_kv(*kv_args, False)
    total = kv_all[0]
    for s in range(1, n):
        total = total + kv_all[s]
    fresh = (total * inv).astype(jnp.bfloat16)
    nk_ref[...] = fresh[:, :width]
    nv_ref[...] = fresh[:, width:]
    fresh = fresh.astype(f32)
    for i in range(2 * heads):
        fresh_s[:, i, :] = fresh[:, i * vdim : (i + 1) * vdim]

    new_scores, new_values = [], []
    for b in range(seqs):
        new_key = doubled(fresh_s[b, :heads])
        new_values.append(doubled(fresh_s[b, heads:]))
        new_scores.append(jnp.sum(queries[b] * new_key, axis=-1, keepdims=True))

    wait_kv(*stat_args, False)

    def stat(s, i):
        return jnp.concatenate([stat_all[s][:, 2 * i + j : 2 * i + j + 1] for j in range(2)], axis=0)

    weighted = []
    for b in range(seqs):
        peaks = [stat(s, b) for s in range(n)]
        top = functools.reduce(jnp.maximum, peaks, new_scores[b])
        factors = [jnp.exp(p - top) for p in peaks]
        new_factor = jnp.exp(new_scores[b] - top)
        whole_sum = new_factor
        for s in range(n):
            whole_sum = whole_sum + stat(s, seqs + b) * factors[s]
        weighted.append((factors, new_factor, whole_sum))
    for b in range(seqs):
        wait_kv(*acc_args[b], False)
    for b in range(seqs):
        factors, new_factor, whole_sum = weighted[b]
        summed = new_values[b] * new_factor
        for s in range(n):
            summed = summed + acc_all[s, b].astype(f32) * factors[s]
        maps = summed / whole_sum
        mixed = maps[:heads] - lam * maps[heads:]
        normed = (
            mixed
            * lax.rsqrt(jnp.mean(mixed * mixed, axis=-1, keepdims=True) + epsilon)
            * hg_s[...]
        )
        head_rows[b] = normed
    flat = jnp.concatenate(
        [head_rows[:, h, :].astype(jnp.bfloat16) for h in range(heads)], axis=-1
    )
    wo_load.wait()
    tp_all[side] = jnp.dot(flat, wo_s[...], preferred_element_type=f32).astype(jnp.bfloat16)
    for o in range(1, ntp):
        pltpu.make_async_remote_copy(
            src_ref=tp_all.at[side], dst_ref=tp_all.at[side],
            send_sem=tp_send.at[o], recv_sem=tp_recv.at[side],
            device_id={"tp": lax.rem(side + o, ntp)}, device_id_type=MESH,
        ).start()
    wait_kv(*q_args, True)
    wait_kv(*kv_args, True)
    wait_kv(*stat_args, True)
    for b in range(seqs):
        wait_kv(*acc_args[b], True)
    for o in range(1, ntp):
        src = lax.rem(side + o, ntp)
        copy = pltpu.make_async_remote_copy(
            src_ref=tp_all.at[src], dst_ref=tp_all.at[src],
            send_sem=tp_send.at[o], recv_sem=tp_recv.at[src],
            device_id={"tp": src}, device_id_type=MESH,
        )
        copy.wait_recv()
        copy.wait_send()
    result = tp_all[0].astype(f32)
    for s in range(1, ntp):
        result = result + tp_all[s].astype(f32)
    out_ref[...] = result.astype(jnp.bfloat16)


def store(a_ref, b_ref, c_ref, a_out, b_out, c_out, sem):
    pairs = ((a_ref, a_out), (b_ref, b_out), (c_ref, c_out))
    copies = [pltpu.make_async_copy(src, dst, sem.at[i]) for i, (src, dst) in enumerate(pairs)]
    for copy in copies:
        copy.start()
    for copy in copies:
        copy.wait()


def per_device(
    n, ntp,
    tokens, norm_gain, w_query, w_key, w_value, w_output,
    key_cache, value_cache, lengths, lam, head_gain,
):
    seqs, features = tokens.shape
    width = w_query.shape[1]
    heads = lam.shape[0]
    vdim = head_gain.shape[0]
    span = key_cache.shape[1]
    columns = w_output.shape[1]
    bf16, f32 = jnp.bfloat16, jnp.float32
    vmem, dma = pltpu.VMEM, pltpu.SemaphoreType.DMA
    keys = key_cache.reshape(seqs, span * heads, vdim)
    values = value_cache.reshape(seqs, span * heads, vdim)
    body = functools.partial(kernel, n, ntp, features * n, vdim // 2)
    shapes = ((seqs, columns), (seqs, width), (seqs, width))
    parts = pl.pallas_call(
        body,
        out_shape=tuple(vmem(shape, bf16) for shape in shapes),
        in_specs=[pl.BlockSpec(memory_space=HBM)] * 11,
        out_specs=(pl.BlockSpec(memory_space=pltpu.VMEM),) * 3,
        scratch_shapes=[
            vmem((seqs, features), bf16),
            vmem((1, features), f32),
            vmem(w_query.shape, bf16),
            vmem(w_key.shape, bf16),
            vmem(w_value.shape, bf16),
            vmem(w_output.shape, bf16),
            vmem(keys.shape, bf16),
            vmem(values.shape, bf16),
            pltpu.SMEM((seqs,), jnp.int32),
            pltpu.SMEM((heads,), f32),
            vmem((1, vdim), f32),
            vmem((n, seqs, width + 128), f32),
            vmem((n, seqs, 2 * width), f32),
            vmem((n, seqs, 2 * heads, vdim), bf16),
            vmem((n, heads, 128), f32),
            vmem((ntp, seqs, columns), bf16),
            vmem((seqs, 2 * heads, span * heads), f32),
            vmem((seqs, heads, vdim), f32),
            vmem((seqs, 2 * heads, vdim), f32),
            vmem((seqs, heads, vdim), f32),
            dma((9,)), dma((seqs,)), dma((seqs,)),
            dma((n,)), dma((n,)), dma((n,)), dma((n,)),
            dma((n, seqs)), dma((n, seqs)), dma((n,)), dma((n,)),
            dma((ntp,)), dma((ntp,)),
        ],
        compiler_params=pltpu.CompilerParams(
            collective_id=0, has_side_effects=True, vmem_limit_bytes=56 * 1024 * 1024
        ),
    )(
        tokens, norm_gain.reshape(1, -1), w_query, w_key, w_value, w_output,
        keys, values, lengths, lam, head_gain.reshape(1, -1),
    )
    return pl.pallas_call(
        store,
        out_shape=tuple(jax.ShapeDtypeStruct(shape, bf16) for shape in shapes),
        in_specs=[pl.BlockSpec(memory_space=pltpu.VMEM)] * 3,
        out_specs=(pl.BlockSpec(memory_space=HBM),) * 3,
        scratch_shapes=[dma((3,))],
        compiler_params=pltpu.CompilerParams(vmem_limit_bytes=1024 * 1024),
    )(*parts)


def solution(mesh):
    in_specs = (
        P("dp", "kv"),
        P("kv"),
        P("kv", "tp"),
        P("kv", "tp"),
        P("kv", "tp"),
        P("tp", "kv"),
        P("dp", "kv", "tp", None),
        P("dp", "kv", "tp", None),
        P("dp"),
        P("tp"),
        P(),
    )
    out_specs = (P("dp", "kv"), P("dp", "tp"), P("dp", "tp"))
    return jax.shard_map(
        functools.partial(per_device, mesh.shape["kv"], mesh.shape["tp"]),
        mesh=mesh, in_specs=in_specs, out_specs=out_specs, check_vma=False,
    )
```

```python
import functools

import jax
import jax.numpy as jnp
from jax import lax
from jax.experimental import pallas as pl
from jax.experimental.pallas import tpu as pltpu
from jax.sharding import PartitionSpec as P

MESH = pl.DeviceIdType.MESH
epsilon = 1e-06
HBM = pltpu.HBM


def kernel(
    n, ntp, d_model, head_width,
    x_hbm, g_hbm, wq_hbm, wk_hbm, wv_hbm, wo_hbm, kc_hbm, vc_hbm, len_hbm, lam_hbm, hg_hbm,
    out_ref, nk_ref, nv_ref,
    x_s, g_s, wq_s, wk_s, wv_s, wo_s, kc_s, vc_s, len_s, lam_s, hg_s,
    q_all, kv_all, acc_all, stat_all, tp_all, bias_s, q_rows, fresh_s, head_rows,
    load_sem, k_sem, v_sem,
    q_send, q_recv, kv_send, kv_recv, acc_send, acc_recv, stat_send, stat_recv, tp_send, tp_recv,
):
    me = lax.axis_index("kv")
    side = lax.axis_index("tp")
    seqs = x_s.shape[0]
    width = wq_s.shape[1]
    vdim = hg_s.shape[1]
    heads = width // vdim
    cols = kc_s.shape[1]
    span = cols // heads
    f32 = jnp.float32

    def load(src, dst, i):
        copy = pltpu.make_async_copy(src, dst, load_sem.at[i])
        copy.start()
        return copy

    x_load = load(x_hbm, x_s, 0)
    g_load = load(g_hbm, g_s, 1)
    wq_load = load(wq_hbm, wq_s, 2)

    def far_peer(o):
        k = o - 1
        down = n - 1 - k - lax.div(me + k, n - 1)
        up = k + lax.div(k - me + n, n)
        return down + lax.div(2 * me, n) * (up - down)

    barrier = pltpu.get_barrier_semaphore()
    for o in range(1, n):
        pl.semaphore_signal(
            barrier, inc=1, device_id={"kv": far_peer(o)}, device_id_type=MESH
        )
    for o in range(1, ntp):
        pl.semaphore_signal(
            barrier, inc=1, device_id={"tp": lax.rem(side + o, ntp)}, device_id_type=MESH
        )

    def send_kv(buf, at, send, recv):
        for o in range(1, n):
            pltpu.make_async_remote_copy(
                src_ref=buf.at[at(me)], dst_ref=buf.at[at(me)],
                send_sem=send(o), recv_sem=recv(me),
                device_id={"kv": far_peer(o)}, device_id_type=MESH,
            ).start()

    def wait_kv(buf, at, send, recv, sent, offsets=range(1, n)):
        for o in offsets:
            src = lax.rem(me + o, n)
            copy = pltpu.make_async_remote_copy(
                src_ref=buf.at[at(src)], dst_ref=buf.at[at(src)],
                send_sem=send(o), recv_sem=recv(src),
                device_id={"kv": src}, device_id_type=MESH,
            )
            if sent:
                copy.wait_send()
            else:
                copy.wait_recv()

    x_load.wait()
    g_load.wait()
    xf = x_s[...].astype(f32)
    squares = jnp.sum(xf * xf, axis=-1, keepdims=True)
    scaled = (xf * g_s[...]).astype(jnp.bfloat16)
    wq_load.wait()
    wk_load = load(wk_hbm, wk_s, 4)
    wv_load = load(wv_hbm, wv_s, 5)
    len_load = load(len_hbm, len_s, 3)
    lam_load = load(lam_hbm, lam_s, 6)
    hg_load = load(hg_hbm, hg_s, 7)
    k_loads, v_loads = [], []
    for b in range(seqs):
        copy = pltpu.make_async_copy(kc_hbm.at[b], kc_s.at[b], k_sem.at[b])
        copy.start()
        k_loads.append(copy)
    for b in range(seqs):
        copy = pltpu.make_async_copy(vc_hbm.at[b], vc_s.at[b], v_sem.at[b])
        copy.start()
        v_loads.append(copy)
    wo_load = load(wo_hbm, wo_s, 8)

    q_all[me, :, :width] = jnp.dot(scaled, wq_s[...], preferred_element_type=f32)
    q_all[me, :, width:] = jnp.broadcast_to(squares, (seqs, q_all.shape[2] - width))
    pl.semaphore_wait(barrier, n - 1 + ntp - 1)
    whole = lambda s: s
    q_args = (q_all, whole, lambda o: q_send.at[o], lambda s: q_recv.at[s])
    kv_args = (kv_all, whole, lambda o: kv_send.at[o], lambda s: kv_recv.at[s])
    stat_args = (stat_all, whole, lambda o: stat_send.at[o], lambda s: stat_recv.at[s])
    acc_args = (acc_all, whole, lambda o: acc_send.at[o], lambda s: acc_recv.at[s])
    send_kv(*q_args)
    wk_load.wait()
    kv_all[me, :, :width] = jnp.dot(scaled, wk_s[...], preferred_element_type=f32)
    wv_load.wait()
    kv_all[me, :, width:] = jnp.dot(scaled, wv_s[...], preferred_element_type=f32)

    len_load.wait()
    lam_load.wait()
    hg_load.wait()
    col = lax.broadcasted_iota(jnp.int32, (2 * heads, cols), 1)
    row = lax.broadcasted_iota(jnp.int32, (2 * heads, cols), 0)
    diagonal = lax.rem(col, heads) == lax.rem(row, heads)
    for b in range(seqs):
        before = (len_s[b] - me * span) * heads
        bias_s[b] = jnp.where(diagonal & (col < before), f32(0.0), f32(-jnp.inf))
    lane = lax.broadcasted_iota(jnp.int32, (2 * heads, vdim), 1)
    half = lax.broadcasted_iota(jnp.int32, (2 * heads, vdim), 0) // heads
    own_map = (lane // head_width) == half

    wait_kv(*q_args, False, range(1, 2))

    send_kv(*kv_args)
    wait_kv(*q_args, False, range(2, n))
    for b in range(seqs):
        k_loads[b].wait()
    total = q_all[0]
    for s in range(1, n):
        total = total + q_all[s]
    inv = lax.rsqrt(total[:, width : width + 1] / d_model + epsilon)
    query = (total[:, :width] * inv).astype(jnp.bfloat16).astype(f32)
    for h in range(heads):
        q_rows[:, h, :] = query[:, h * vdim : (h + 1) * vdim]

    def doubled(rows):
        return jnp.concatenate([rows, rows], axis=0)

    queries = [
        jnp.where(own_map, doubled(q_rows[b]), f32(0.0)) * head_width**-0.5 for b in range(seqs)
    ]
    stats = jnp.zeros(stat_all.shape[1:], f32)
    stat_lane = lax.broadcasted_iota(jnp.int32, stats.shape, 1)
    rounded = []
    for b in range(seqs):
        score = (
            lax.dot_general(
                queries[b].astype(jnp.bfloat16), kc_s[b],
                (((1,), (1,)), ((), ())), preferred_element_type=f32,
            )
            + bias_s[b]
        )
        peak = jnp.maximum(jnp.max(score, axis=-1, keepdims=True), f32(-1e30))
        weights = jnp.exp(score - peak)
        block_sum = jnp.sum(weights, axis=-1, keepdims=True)
        rounded.append(weights.astype(jnp.bfloat16))
        for j in range(2):
            rows = slice(j * heads, (j + 1) * heads)
            stats = jnp.where(stat_lane == 2 * b + j, peak[rows], stats)
            stats = jnp.where(stat_lane == 2 * (seqs + b) + j, block_sum[rows], stats)
    stat_all[me] = stats
    send_kv(*stat_args)
    for b in range(seqs):
        v_loads[b].wait()
    for b in range(seqs):
        acc = jnp.dot(rounded[b], vc_s[b], preferred_element_type=f32)
        acc_all[me, b] = acc.astype(acc_all.dtype)
        if b == seqs - 1:
            send_kv(*acc_args)

    h_row = lax.broadcasted_iota(jnp.int32, (heads, 1), 0)
    lam = jnp.zeros((heads, 1), f32)
    for h in range(heads):
        lam = jnp.where(h_row == h, lam_s[h], lam)

    wait_kv(*kv_args, False)
    total = kv_all[0]
    for s in range(1, n):
        total = total + kv_all[s]
    fresh = (total * inv).astype(jnp.bfloat16)
    nk_ref[...] = fresh[:, :width]
    nv_ref[...] = fresh[:, width:]
    fresh = fresh.astype(f32)
    for i in range(2 * heads):
        fresh_s[:, i, :] = fresh[:, i * vdim : (i + 1) * vdim]

    new_scores, new_values = [], []
    for b in range(seqs):
        new_key = doubled(fresh_s[b, :heads])
        new_values.append(doubled(fresh_s[b, heads:]))
        new_scores.append(jnp.sum(queries[b] * new_key, axis=-1, keepdims=True))

    wait_kv(*stat_args, False)

    def stat(s, i):
        return jnp.concatenate([stat_all[s][:, 2 * i + j : 2 * i + j + 1] for j in range(2)], axis=0)

    weighted = []
    for b in range(seqs):
        peaks = [stat(s, b) for s in range(n)]
        top = functools.reduce(jnp.maximum, peaks, new_scores[b])
        factors = [jnp.exp(p - top) for p in peaks]
        new_factor = jnp.exp(new_scores[b] - top)
        whole_sum = new_factor
        for s in range(n):
            whole_sum = whole_sum + stat(s, seqs + b) * factors[s]
        weighted.append((factors, new_factor, whole_sum))
    for b in range(seqs):
        if b == 0:
            wait_kv(*acc_args, False)
    for b in range(seqs):
        factors, new_factor, whole_sum = weighted[b]
        summed = new_values[b] * new_factor
        for s in range(n):
            summed = summed + acc_all[s, b].astype(f32) * factors[s]
        maps = summed / whole_sum
        mixed = maps[:heads] - lam * maps[heads:]
        normed = (
            mixed
            * lax.rsqrt(jnp.mean(mixed * mixed, axis=-1, keepdims=True) + epsilon)
            * hg_s[...]
        )
        head_rows[b] = normed
    flat = jnp.concatenate(
        [head_rows[:, h, :].astype(jnp.bfloat16) for h in range(heads)], axis=-1
    )
    wo_load.wait()
    tp_all[side] = jnp.dot(flat, wo_s[...], preferred_element_type=f32).astype(jnp.bfloat16)
    for o in range(1, ntp):
        pltpu.make_async_remote_copy(
            src_ref=tp_all.at[side], dst_ref=tp_all.at[side],
            send_sem=tp_send.at[o], recv_sem=tp_recv.at[side],
            device_id={"tp": lax.rem(side + o, ntp)}, device_id_type=MESH,
        ).start()
    wait_kv(*q_args, True)
    wait_kv(*kv_args, True)
    wait_kv(*stat_args, True)
    for b in range(seqs):
        if b == 0:
            wait_kv(*acc_args, True)
    for o in range(1, ntp):
        src = lax.rem(side + o, ntp)
        copy = pltpu.make_async_remote_copy(
            src_ref=tp_all.at[src], dst_ref=tp_all.at[src],
            send_sem=tp_send.at[o], recv_sem=tp_recv.at[src],
            device_id={"tp": src}, device_id_type=MESH,
        )
        copy.wait_recv()
        copy.wait_send()
    result = tp_all[0].astype(f32)
    for s in range(1, ntp):
        result = result + tp_all[s].astype(f32)
    out_ref[...] = result.astype(jnp.bfloat16)


def store(a_ref, b_ref, c_ref, a_out, b_out, c_out, sem):
    pairs = ((a_ref, a_out), (b_ref, b_out), (c_ref, c_out))
    copies = [pltpu.make_async_copy(src, dst, sem.at[i]) for i, (src, dst) in enumerate(pairs)]
    for copy in copies:
        copy.start()
    for copy in copies:
        copy.wait()


def per_device(
    n, ntp,
    tokens, norm_gain, w_query, w_key, w_value, w_output,
    key_cache, value_cache, lengths, lam, head_gain,
):
    seqs, features = tokens.shape
    width = w_query.shape[1]
    heads = lam.shape[0]
    vdim = head_gain.shape[0]
    span = key_cache.shape[1]
    columns = w_output.shape[1]
    bf16, f32 = jnp.bfloat16, jnp.float32
    vmem, dma = pltpu.VMEM, pltpu.SemaphoreType.DMA
    keys = key_cache.reshape(seqs, span * heads, vdim)
    values = value_cache.reshape(seqs, span * heads, vdim)
    body = functools.partial(kernel, n, ntp, features * n, vdim // 2)
    shapes = ((seqs, columns), (seqs, width), (seqs, width))
    parts = pl.pallas_call(
        body,
        out_shape=tuple(vmem(shape, bf16) for shape in shapes),
        in_specs=[pl.BlockSpec(memory_space=HBM)] * 11,
        out_specs=(pl.BlockSpec(memory_space=pltpu.VMEM),) * 3,
        scratch_shapes=[
            vmem((seqs, features), bf16),
            vmem((1, features), f32),
            vmem(w_query.shape, bf16),
            vmem(w_key.shape, bf16),
            vmem(w_value.shape, bf16),
            vmem(w_output.shape, bf16),
            vmem(keys.shape, bf16),
            vmem(values.shape, bf16),
            pltpu.SMEM((seqs,), jnp.int32),
            pltpu.SMEM((heads,), f32),
            vmem((1, vdim), f32),
            vmem((n, seqs, width + 128), f32),
            vmem((n, seqs, 2 * width), f32),
            vmem((n, seqs, 2 * heads, vdim), bf16),
            vmem((n, heads, 128), f32),
            vmem((ntp, seqs, columns), bf16),
            vmem((seqs, 2 * heads, span * heads), f32),
            vmem((seqs, heads, vdim), f32),
            vmem((seqs, 2 * heads, vdim), f32),
            vmem((seqs, heads, vdim), f32),
            dma((9,)), dma((seqs,)), dma((seqs,)),
            dma((n,)), dma((n,)), dma((n,)), dma((n,)),
            dma((n,)), dma((n,)), dma((n,)), dma((n,)),
            dma((ntp,)), dma((ntp,)),
        ],
        compiler_params=pltpu.CompilerParams(
            collective_id=0, has_side_effects=True, vmem_limit_bytes=56 * 1024 * 1024
        ),
    )(
        tokens, norm_gain.reshape(1, -1), w_query, w_key, w_value, w_output,
        keys, values, lengths, lam, head_gain.reshape(1, -1),
    )
    return pl.pallas_call(
        store,
        out_shape=tuple(jax.ShapeDtypeStruct(shape, bf16) for shape in shapes),
        in_specs=[pl.BlockSpec(memory_space=pltpu.VMEM)] * 3,
        out_specs=(pl.BlockSpec(memory_space=HBM),) * 3,
        scratch_shapes=[dma((3,))],
        compiler_params=pltpu.CompilerParams(vmem_limit_bytes=1024 * 1024),
    )(*parts)


def solution(mesh):
    in_specs = (
        P("dp", "kv"),
        P("kv"),
        P("kv", "tp"),
        P("kv", "tp"),
        P("kv", "tp"),
        P("tp", "kv"),
        P("dp", "kv", "tp", None),
        P("dp", "kv", "tp", None),
        P("dp"),
        P("tp"),
        P(),
    )
    out_specs = (P("dp", "kv"), P("dp", "tp"), P("dp", "tp"))
    return jax.shard_map(
        functools.partial(per_device, mesh.shape["kv"], mesh.shape["tp"]),
        mesh=mesh, in_specs=in_specs, out_specs=out_specs, check_vma=False,
    )
```
